32 devices in a mesh: grp: 2 (over x), ep: 16 (over z, y, core).
Axes of the slice: x: 2, y: 2, z: 4, core: 2. Of those that a mesh axis runs over, the one named last changes fastest.
Arguments:
- hidden: bfloat16 [96, 2048], P(('grp', 'ep')), parts along dimension 0, may hold values from -6 to 6
- conv_window: bfloat16 [96, 3, 6144], P(('grp', 'ep')), parts along dimension 0, may hold values from -6 to 6
- ssm_state: float32 [96, 64, 64, 128], P(('grp', 'ep')), parts along dimension 0, may hold values from -1.75 to 1.75
- gate_proj: bfloat16 [2048, 4096], P(None, 'ep'), may hold values from -0.125 to 0.125
- input_proj: bfloat16 [2048, 4096], P(None, 'ep'), may hold values from -0.125 to 0.125
- write_proj: bfloat16 [2048, 1024], P(None, 'ep'), may hold values from -0.125 to 0.125
- read_proj: bfloat16 [2048, 1024], P(None, 'ep'), may hold values from -0.125 to 0.125
- step_proj: bfloat16 [2048, 64], replicated, may hold values from -0.125 to 0.125
- step_bias: float32 [64], replicated, may hold values from -2 to 1
- decay_log: float32 [64], replicated, may hold values from -2.3 to 1.4
- decay_shift: float32 [96, 64], P(('grp', 'ep')), parts along dimension 0, may hold values from -0.7 to 0
- skip_scale: float32 [64], replicated, may hold values from -4 to 4
- conv_taps: bfloat16 [4, 6144], replicated, may hold values from -3 to 3
- conv_bias: float32 [6144], replicated, may hold values from -3 to 3
- mix_gain: float32 [2048], replicated, may hold values from 0.1 to 1.9
- group_gain: float32 [4096], replicated, may hold values from 0.1 to 1.9
- out_proj: bfloat16 [4096, 2048], P(None, 'ep'), may hold values from -0.09375 to 0.09375
- ffn_gain: float32 [2048], replicated, may hold values from 0.1 to 1.9
- router: bfloat16 [2048, 16], replicated, may hold values from -0.125 to 0.125
- expert_ids: int32 [96, 6], P(('grp', 'ep')), parts along dimension 0, may hold values from 0 to 15, all different within a row; in each aligned block of 3 rows (0 to 2, 3 to 5, ...) at most 2 rows name the same one
- expert_gate: bfloat16 [16, 2048, 512], P('ep'), may hold values from -0.125 to 0.125
- expert_up: bfloat16 [16, 2048, 512], P('ep'), may hold values from -0.125 to 0.125
- expert_down: bfloat16 [16, 512, 2048], P('ep'), may hold values from -0.25 to 0.25
- shared_gate: bfloat16 [2048, 512], P('ep'), may hold values from -0.125 to 0.125
- shared_up: bfloat16 [2048, 512], P('ep'), may hold values from -0.125 to 0.125
- shared_down: bfloat16 [512, 2048], replicated, may hold values from -0.25 to 0.25
Outputs:
- layer_out: bfloat16 [96, 2048], P(('grp', 'ep')), parts along dimension 0
- next_state: float32 [96, 64, 64, 128], P(('grp', 'ep')), parts along dimension 0
- next_window: bfloat16 [96, 3, 6144], P(('grp', 'ep')), parts along dimension 0
The draws below stay inside these ranges and needn't reach their ends.
There are 2 independent parts, one for each index of `grp`. The reference program is written for one: setup_inputs(seed, part) draws one part's arguments, and reference() takes and returns one part's arrays. A program takes and returns all parts, laid end to end along the dimension named above; an argument that names none is the same for every part. Nothing has to cross between parts.
Inputs may be any that keep to these rules, and one draw needn't show every extreme that they name: `expert_ids`: each row names 6 different experts; in the rows of one device no expert is named by more than 2 rows, and in every draw some device's rows name some expert exactly 2 times.
All inputs are finite; a program needn't handle non-finite values.
Results may differ from the reference program's by a relative error of at most 0.019.
Values may be sent and summed in bfloat16 or wider, within the bound.
A program may use at most 128 MiB of HBM per device.

```python
import math
import jax
import jax.numpy as jnp
import numpy as np
from jax import lax

D = 2048
INNER = 4096
HEAD_DIM = 64
GROUPS = 8
STATE = 128
CONV = 4
EFF = 512
SFF = 512
TOP_K = 6
SEQ_DEV = 3
CAP = 2
HEADS = 64
CONV_DIM = 6144
EXPERTS = 16
SEQS = 48


def block_levels(own_key, extent, shards, low, largest):
    loudness, own = 1.0, jax.random.fold_in(own_key, 6)
    for dim, shards_of in shards:
        draws = jnp.exp(jax.random.uniform(jax.random.fold_in(own, dim), (shards_of,), jnp.float32, low / len(shards), largest / len(shards)))
        loudness = loudness * jnp.repeat(draws, extent[dim] // shards_of).reshape([-1 if axis == dim else 1 for axis in range(len(extent))])
    return loudness


def routed_block(rng, own, number, rows, amount, top, limit, slope):
    order = jax.random.permutation(rng, amount)
    packed, ordinary = shares(amount, rows * top, limit, slope, True), shares(amount, rows * top, limit, slope, False)
    places = jnp.arange(amount)

    def named(lengths, offset_by):
        used = int((lengths > 0).sum())
        fixed = max(1, used // 4)
        passed = fixed + (places - fixed + offset_by * (used - fixed)) % max(1, amount - fixed)
        return jnp.zeros((amount,), jnp.int32).at[order[jnp.where(places < fixed, places, passed)]].set(jnp.asarray(lengths, jnp.int32))

    lengths = jnp.where(number % 4 == 0, named(packed, number // 4), named(ordinary, number - number // 4 - 1))
    mixed = jax.random.permutation(jax.random.fold_in(own, 3), amount)
    source_of, sink = mixed[0:amount // 2 * 2:2], mixed[1:amount // 2 * 2:2]
    slack = jnp.minimum(lengths[source_of] - 1, limit - lengths[sink]) // 2
    slack = jnp.where((source_of == order[0]) | (sink == order[0]) | (lengths[sink] == 0), 0, jnp.maximum(slack, 0))
    passed = jax.random.randint(jax.random.fold_in(own, 4), (amount // 2,), 0, 1 << 20) % (slack + 1)
    lengths = lengths.at[source_of].add(-passed).at[sink].add(passed)
    labels = jnp.searchsorted(jnp.cumsum(lengths), jnp.arange(rows * top), side="right").astype(jnp.int32)
    listing = labels.reshape(top, rows).T
    listing = listing[jax.random.permutation(jax.random.fold_in(own, 1), rows)]
    offset_by = jax.random.randint(jax.random.fold_in(own, 2), (rows, 1), 0, top)
    return jnp.take_along_axis(listing, (jnp.arange(top)[None, :] + offset_by) % top, axis=1)


def shares(count, total, most, lean, full):
    portions = [(1 << 20) // math.isqrt(grade ** lean) + 1 for grade in range(1, count + 1)]
    largest = most if full else min(most, max(-(-total // count), total * portions[0] // sum(portions)))
    least = 1 if total - largest >= count - 1 else 0
    given, rest = [largest] + [least] * (count - 1), total - largest - least * (count - 1)
    while rest > 0:
        free = [i for i in range(1, count) if given[i] < largest] or [i for i in range(1, count) if given[i] < most]
        pool, budget = sum([portions[i] for i in free]), rest
        for i in free:
            addition = min(most - given[i], max(1, budget * portions[i] // pool), rest)
            given[i] = given[i] + addition
            rest = rest - addition
    return np.array(given)


def gaussian(key, extent, deviation, most, pieces=(), held_as=jnp.bfloat16):
    values = deviation * jax.random.normal(key, extent, jnp.float32)
    if pieces:
        values = values * block_levels(key, extent, pieces, -0.22, 0.18)
    return jnp.clip(values, -most, most).astype(held_as)


def setup_inputs(seed: int = 0, part: int = 0) -> dict:
    seeds = jax.random.split(jax.random.key(seed), 27)
    part_keys = jax.random.split(jax.random.fold_in(seeds[26], part), 27)
    hidden = gaussian(part_keys[0], (SEQS, D), 1.0, 6.0, ((0, 16),))
    conv_window = gaussian(part_keys[1], (SEQS, CONV - 1, CONV_DIM), 1.0, 6.0, ((0, 16),))
    ssm_state = gaussian(part_keys[2], (SEQS, HEADS, HEAD_DIM, STATE), 0.3, 1.75, ((0, 16),), jnp.float32)
    gate_proj = gaussian(seeds[3], (D, INNER), D ** -0.5, 0.125, ((1, 16),))
    input_proj = gaussian(seeds[4], (D, INNER), D ** -0.5, 0.125, ((1, 16),))
    write_proj = gaussian(seeds[5], (D, GROUPS * STATE), D ** -0.5, 0.125, ((1, 16),))
    read_proj = gaussian(seeds[6], (D, GROUPS * STATE), D ** -0.5, 0.125, ((1, 16),))
    step_proj = gaussian(seeds[7], (D, HEADS), D ** -0.5, 0.125)
    step_bias = jnp.clip(jax.random.uniform(seeds[8], (HEADS,), jnp.float32, -2.0, 1.0), -2.0, 1.0)
    decay_log = jnp.clip(jax.random.uniform(seeds[9], (HEADS,), jnp.float32, -2.3, 1.4), -2.3, 1.4)
    decay_shift = jnp.clip(-0.7 + 0.7 * jax.random.uniform(part_keys[10], (SEQS, HEADS), jnp.float32) ** block_levels(part_keys[10], (SEQS, HEADS), ((0, 16),), -0.2, 0.2), -0.7, 0.0)
    skip_scale = gaussian(seeds[11], (HEADS,), 1.0, 4.0, (), jnp.float32)
    conv_taps = gaussian(seeds[12], (CONV, CONV_DIM), CONV ** -0.5, 3.0)
    conv_bias = gaussian(seeds[13], (CONV_DIM,), 0.5, 3.0, (), jnp.float32)
    mix_gain = jnp.clip(1.0 + 0.18 * jax.random.normal(seeds[14], (D,), jnp.float32), 0.1, 1.9)
    group_gain = jnp.clip(1.0 + 0.18 * jax.random.normal(seeds[15], (INNER,), jnp.float32), 0.1, 1.9)
    out_proj = gaussian(seeds[16], (INNER, D), INNER ** -0.5, 0.09375, ((1, 16),))
    ffn_gain = jnp.clip(1.0 + 0.18 * jax.random.normal(seeds[17], (D,), jnp.float32), 0.1, 1.9)
    router = gaussian(seeds[18], (D, EXPERTS), D ** -0.5, 0.125)
    expert_ids_keys = jax.random.split(jax.random.fold_in(part_keys[19], 1), SEQS // SEQ_DEV)
    expert_ids_turns = jax.random.permutation(jax.random.fold_in(part_keys[19], 3), SEQS // SEQ_DEV)
    expert_ids = jax.vmap(lambda own, number: routed_block(jax.random.fold_in(part_keys[19], 2), own, number, SEQ_DEV, EXPERTS, TOP_K, CAP, 2))(expert_ids_keys, expert_ids_turns).reshape((SEQS, TOP_K))
    expert_gate = gaussian(seeds[20], (EXPERTS, D, EFF), D ** -0.5, 0.125, ((0, 16),))
    expert_up = gaussian(seeds[21], (EXPERTS, D, EFF), D ** -0.5, 0.125, ((0, 16),))
    expert_down = gaussian(seeds[22], (EXPERTS, EFF, D), EFF ** -0.5, 0.25, ((0, 16),))
    shared_gate = gaussian(seeds[23], (D, SFF), D ** -0.5, 0.125, ((0, 16),))
    shared_up = gaussian(seeds[24], (D, SFF), D ** -0.5, 0.125, ((0, 16),))
    shared_down = gaussian(seeds[25], (SFF, D), SFF ** -0.5, 0.25)
    return {"hidden": hidden, "conv_window": conv_window, "ssm_state": ssm_state, "gate_proj": gate_proj, "input_proj": input_proj, "write_proj": write_proj, "read_proj": read_proj, "step_proj": step_proj, "step_bias": step_bias, "decay_log": decay_log, "decay_shift": decay_shift, "skip_scale": skip_scale, "conv_taps": conv_taps, "conv_bias": conv_bias, "mix_gain": mix_gain, "group_gain": group_gain, "out_proj": out_proj, "ffn_gain": ffn_gain, "router": router, "expert_ids": expert_ids, "expert_gate": expert_gate, "expert_up": expert_up, "expert_down": expert_down, "shared_gate": shared_gate, "shared_up": shared_up, "shared_down": shared_down}


epsilon = 1e-06
routed_scale = 2.5

def row_scale(values):
    return lax.rsqrt(lax.optimization_barrier(jnp.mean(values * values, axis=-1, keepdims=True)) + epsilon)

def matmul(left, right):
    return jnp.dot(left, right, preferred_element_type=jnp.float32)

def reference(hidden, conv_window, ssm_state, gate_proj, input_proj, write_proj, read_proj, step_proj, step_bias, decay_log, decay_shift, skip_scale, conv_taps, conv_bias, mix_gain, group_gain, out_proj, ffn_gain, router, expert_ids, expert_gate, expert_up, expert_down, shared_gate, shared_up, shared_down):
    batch_rows = hidden.shape[0]
    head_count = step_bias.shape[0]
    per_group = head_count // GROUPS
    inner_width = gate_proj.shape[1]
    state_span = GROUPS * STATE
    hidden_wide = hidden.astype(jnp.float32)
    normed = (hidden_wide * row_scale(hidden_wide) * mix_gain).astype(jnp.bfloat16)
    gate_rows = matmul(normed, gate_proj).astype(jnp.bfloat16)
    input_rows = matmul(normed, input_proj).astype(jnp.bfloat16)
    write_rows = matmul(normed, write_proj).astype(jnp.bfloat16)
    read_rows = matmul(normed, read_proj).astype(jnp.bfloat16)
    step_raw = matmul(normed, step_proj)
    fresh_row = jnp.concatenate([input_rows, write_rows, read_rows], axis=1)
    window = jnp.concatenate([conv_window, fresh_row[:, None, :]], axis=1)
    convolved = jax.nn.silu(lax.optimization_barrier(jnp.sum(window.astype(jnp.float32) * conv_taps.astype(jnp.float32)[None], axis=1)) + conv_bias)
    head_input = convolved[:, :inner_width].reshape(batch_rows, GROUPS, per_group, HEAD_DIM)
    write_vec = convolved[:, inner_width:inner_width + state_span].reshape(batch_rows, GROUPS, STATE)
    read_vec = convolved[:, inner_width + state_span:].reshape(batch_rows, GROUPS, STATE)
    step_size = jax.nn.softplus(step_raw + step_bias)
    decay_rate = jnp.exp(decay_shift - step_size * jnp.exp(decay_log)).reshape(batch_rows, GROUPS, per_group)
    step_group = step_size.reshape(batch_rows, GROUPS, per_group)
    carried = ssm_state.reshape(batch_rows, GROUPS, per_group, HEAD_DIM, STATE)
    next_state = decay_rate[..., None, None] * carried + (step_group[..., None] * head_input)[..., None] * write_vec[:, :, None, None, :]
    mixed_out = jnp.einsum('sgepn,sgn->sgep', next_state, read_vec, precision=lax.Precision.HIGHEST)
    mixed_out = mixed_out + skip_scale.reshape(GROUPS, per_group)[None, :, :, None] * head_input
    mixed_out = mixed_out.reshape(batch_rows, inner_width).astype(jnp.bfloat16)
    gated_out = mixed_out.astype(jnp.float32) * jax.nn.silu(gate_rows.astype(jnp.float32))
    blocks = gated_out.reshape(batch_rows, GROUPS, -1)
    gated_out = ((blocks * row_scale(blocks)).reshape(batch_rows, inner_width) * group_gain).astype(jnp.bfloat16)
    resid = (hidden_wide + matmul(gated_out, out_proj)).astype(jnp.bfloat16)
    resid_wide = resid.astype(jnp.float32)
    norm_scale = row_scale(resid_wide)
    routed_in = (resid_wide * norm_scale * ffn_gain).astype(jnp.bfloat16)
    shared_in = (resid_wide * ffn_gain).astype(jnp.bfloat16)
    scores = jax.nn.sigmoid(matmul(routed_in, router))
    picked = jnp.take_along_axis(scores, expert_ids, axis=1)
    weights = routed_scale * picked / lax.optimization_barrier(jnp.sum(picked, axis=1, keepdims=True))

    def add_expert(running, inputs):
        weight_gate, weight_up, weight_down, index = inputs
        expert_hidden = (jax.nn.silu(matmul(routed_in, weight_gate)) * matmul(routed_in, weight_up)).astype(jnp.bfloat16)
        result = matmul(expert_hidden, weight_down).astype(jnp.bfloat16)
        coefficient = lax.optimization_barrier(jnp.sum(jnp.where(expert_ids == index, weights, 0.0), axis=1))
        return (running + coefficient[:, None] * result.astype(jnp.float32), None)
    routed, _ = lax.scan(add_expert, jnp.zeros((batch_rows, hidden.shape[1]), jnp.float32), (expert_gate, expert_up, expert_down, jnp.arange(expert_gate.shape[0], dtype=jnp.int32)))
    shared_hidden = (jax.nn.silu(norm_scale * matmul(shared_in, shared_gate)) * (norm_scale * matmul(shared_in, shared_up))).astype(jnp.bfloat16)
    layer_out = (resid_wide + routed + matmul(shared_hidden, shared_down)).astype(jnp.bfloat16)
    return (layer_out, next_state.reshape(ssm_state.shape), window[:, 1:])
```

```python
import functools

import jax
import jax.numpy as jnp
from jax import lax
from jax.experimental import pallas as pl
from jax.experimental.pallas import tpu as pltpu
from jax.sharding import PartitionSpec as P

HEAD_DIM = 64
GROUPS = 8
STATE = 128


epsilon = 1e-06
routed_scale = 2.5


def row_scale(values):
    return lax.rsqrt(jnp.mean(values * values, axis=-1, keepdims=True) + epsilon)


def matmul(left, right):
    return jnp.dot(left, right, preferred_element_type=jnp.float32)


def expert_result(rows_in, weight_gate, weight_up, weight_down):
    expert_hidden = (jax.nn.silu(matmul(rows_in, weight_gate)) * matmul(rows_in, weight_up)).astype(
        jnp.bfloat16
    )
    return matmul(expert_hidden, weight_down).astype(jnp.bfloat16)


def exchange(blocks, ident):
    return lax.all_to_all(blocks, "ep", split_axis=0, concat_axis=0, tiled=True)


def gather(block, ident):
    return exchange(jnp.broadcast_to(block[None], (lax.axis_size("ep"),) + block.shape), ident)


def state_kernel(per_group, decay, inputs, write, read, carried, updated, mixed):
    row, part = pl.program_id(0), pl.program_id(1)
    heads = carried.shape[1]
    scaled = inputs[0, 0]
    lane = lax.broadcasted_iota(jnp.int32, scaled.shape, 1)
    total = jnp.zeros(scaled.shape, jnp.float32)
    for head in range(heads):
        group = head // per_group
        fresh = (
            carried[0, head] * decay[row, part * heads + head]
            + scaled[:, head : head + 1] * write[0, 0, group : group + 1]
        )
        updated[0, head] = fresh
        column = jnp.sum(fresh * read[0, 0, group : group + 1], axis=1, keepdims=True)
        total = jnp.where(lane == head, column, total)
    mixed[0, 0] = total


def state_step(state, decay_rate, scaled, write_vec, read_vec):
    rows, head_count, head_dim, entries = state.shape
    groups = write_vec.shape[1]
    parts = 2
    heads = head_count // parts
    inputs = scaled.reshape(rows, parts, heads, head_dim).transpose(0, 1, 3, 2)
    vec_shape = (rows, parts, groups // parts, entries)
    part_spec = lambda *dims: pl.BlockSpec((1, 1) + dims, lambda row, part: (row, part, 0, 0))
    state_spec = pl.BlockSpec((1, heads, head_dim, entries), lambda row, part: (row, part, 0, 0))
    next_state, mixed = pl.pallas_call(
        functools.partial(state_kernel, head_count // groups),
        grid=(rows, parts),
        out_shape=(
            jax.ShapeDtypeStruct(state.shape, jnp.float32),
            jax.ShapeDtypeStruct(inputs.shape, jnp.float32),
        ),
        in_specs=[
            pl.BlockSpec(memory_space=pltpu.SMEM),
            part_spec(head_dim, heads),
            part_spec(groups // parts, entries),
            part_spec(groups // parts, entries),
            state_spec,
        ],
        out_specs=(state_spec, part_spec(head_dim, heads)),
    )(decay_rate, inputs, write_vec.reshape(vec_shape), read_vec.reshape(vec_shape), state)
    return next_state, mixed.transpose(0, 1, 3, 2).reshape(rows, head_count, head_dim)


def shards(
    hidden,
    conv_window,
    ssm_state,
    gate_proj,
    input_proj,
    write_proj,
    read_proj,
    step_proj,
    step_bias,
    decay_log,
    decay_shift,
    skip_scale,
    conv_taps,
    conv_bias,
    mix_gain,
    group_gain,
    out_proj,
    ffn_gain,
    router,
    expert_ids,
    expert_gate,
    expert_up,
    expert_down,
    shared_gate,
    shared_up,
    shared_down,
):
    local_rows = hidden.shape[0]
    device_index = lax.axis_index("ep")
    width = hidden.shape[1]
    first_row = device_index * local_rows
    gathered = gather(hidden, 0).reshape(-1, width)
    gathered_wide = gathered.astype(jnp.float32)
    normed = (gathered_wide * row_scale(gathered_wide) * mix_gain).astype(jnp.bfloat16)
    parts = [matmul(normed, proj).astype(jnp.bfloat16) for proj in (gate_proj, input_proj, write_proj, read_proj)]
    outbound = jnp.concatenate(parts, axis=1)
    arrived = exchange(outbound.reshape(-1, local_rows, outbound.shape[1]), 1)
    rows, offset = [], 0
    for part in parts:
        piece = arrived[:, :, offset : offset + part.shape[1]]
        rows.append(piece.transpose(1, 0, 2).reshape(local_rows, -1))
        offset += part.shape[1]
    gate_rows, input_rows, write_rows, read_rows = rows
    hidden_wide = hidden.astype(jnp.float32)
    normed_local = (hidden_wide * row_scale(hidden_wide) * mix_gain).astype(jnp.bfloat16)
    step_raw = matmul(normed_local, step_proj)
    inner_width = gate_rows.shape[1]
    state_span = GROUPS * STATE
    head_count = step_bias.shape[0]
    fresh_row = jnp.concatenate([input_rows, write_rows, read_rows], axis=1)
    window = jnp.concatenate([conv_window, fresh_row[:, None, :]], axis=1)
    convolved = jax.nn.silu(
        jnp.sum(window.astype(jnp.float32) * conv_taps.astype(jnp.float32)[None], axis=1)
        + conv_bias
    )
    head_input = convolved[:, :inner_width].reshape(local_rows, head_count, HEAD_DIM)
    write_vec = convolved[:, inner_width : inner_width + state_span].reshape(
        local_rows, GROUPS, STATE
    )
    read_vec = convolved[:, inner_width + state_span :].reshape(local_rows, GROUPS, STATE)
    step_size = jax.nn.softplus(step_raw + step_bias)
    decay_rate = jnp.exp(decay_shift - step_size * jnp.exp(decay_log))
    next_state, mixed_out = state_step(
        ssm_state, decay_rate, step_size[:, :, None] * head_input, write_vec, read_vec
    )
    mixed_out = mixed_out + skip_scale[None, :, None] * head_input
    mixed_out = mixed_out.reshape(local_rows, inner_width).astype(jnp.bfloat16)
    gated_out = mixed_out.astype(jnp.float32) * jax.nn.silu(gate_rows.astype(jnp.float32))
    blocks = gated_out.reshape(local_rows, GROUPS, -1)
    gated_out = ((blocks * row_scale(blocks)).reshape(local_rows, inner_width) * group_gain).astype(
        jnp.bfloat16
    )
    col_width = out_proj.shape[1]
    resid_cols = lax.dynamic_slice_in_dim(gathered_wide, device_index * col_width, col_width, 1)
    resid_part = (
        resid_cols + matmul(gather(gated_out, 2).reshape(-1, inner_width), out_proj)
    ).astype(jnp.bfloat16)
    resid_all = gather(resid_part, 3).transpose(1, 0, 2).reshape(-1, width)
    gain_part = lax.dynamic_slice_in_dim(ffn_gain, device_index * col_width, col_width, 0)
    shared_part = (resid_part.astype(jnp.float32) * gain_part).astype(jnp.bfloat16)
    shared_pre = jnp.concatenate(
        [matmul(shared_part, shared_gate), matmul(shared_part, shared_up)], axis=1
    ).astype(jnp.bfloat16)
    resid_all_wide = resid_all.astype(jnp.float32)
    scale_all = row_scale(resid_all_wide)
    routed_all = (resid_all_wide * scale_all * ffn_gain).astype(jnp.bfloat16)
    result = expert_result(routed_all, expert_gate[0], expert_up[0], expert_down[0])
    back = exchange(
        jnp.concatenate([result, shared_pre], axis=1).reshape(
            -1, local_rows, width + shared_pre.shape[1]
        ),
        4,
    ).astype(jnp.float32)
    resid_wide = lax.dynamic_slice_in_dim(resid_all_wide, first_row, local_rows, 0)
    norm_scale = lax.dynamic_slice_in_dim(scale_all, first_row, local_rows, 0)
    routed_in = lax.dynamic_slice_in_dim(routed_all, first_row, local_rows, 0)
    scores = jax.nn.sigmoid(matmul(routed_in, router))
    chosen = jnp.any(
        expert_ids[:, :, None] == jnp.arange(router.shape[1], dtype=jnp.int32)[None, None, :], axis=1
    )
    scores = jnp.where(chosen, scores, 0.0)
    weights = routed_scale * scores / jnp.sum(scores, axis=1, keepdims=True)
    routed = jnp.sum(back[:, :, :width] * weights.T[:, :, None], axis=0)
    shared_sum = jnp.sum(back[:, :, width:], axis=0)
    hidden_units = shared_down.shape[0]
    shared_hidden = (
        jax.nn.silu(norm_scale * shared_sum[:, :hidden_units])
        * (norm_scale * shared_sum[:, hidden_units:])
    ).astype(jnp.bfloat16)
    layer_out = (resid_wide + routed + matmul(shared_hidden, shared_down)).astype(jnp.bfloat16)
    return (layer_out, next_state, window[:, 1:])


def solution(mesh):
    placed = (
        P(("grp", "ep"), None),
        P(("grp", "ep"), None, None),
        P(("grp", "ep"), None, None, None),
        P(None, "ep"),
        P(None, "ep"),
        P(None, "ep"),
        P(None, "ep"),
        P(),
        P(),
        P(),
        P(("grp", "ep"), None),
        P(),
        P(),
        P(),
        P(),
        P(),
        P(None, "ep"),
        P(),
        P(),
        P(("grp", "ep"), None),
        P("ep", None, None),
        P("ep", None, None),
        P("ep", None, None),
        P("ep", None),
        P("ep", None),
        P(),
    )
    return jax.shard_map(
        shards,
        mesh=mesh,
        in_specs=placed,
        out_specs=(
            P(("grp", "ep"), None),
            P(("grp", "ep"), None, None, None),
            P(("grp", "ep"), None, None),
        ),
        check_vma=False,
    )
```

```python
import functools

import jax
import jax.numpy as jnp
from jax import lax
from jax.experimental import pallas as pl
from jax.experimental.pallas import tpu as pltpu
from jax.sharding import PartitionSpec as P

HEAD_DIM = 64
GROUPS = 8
STATE = 128


epsilon = 1e-06
routed_scale = 2.5


def row_scale(values):
    return lax.rsqrt(jnp.mean(values * values, axis=-1, keepdims=True) + epsilon)


def matmul(left, right):
    return jnp.dot(left, right, preferred_element_type=jnp.float32)


def expert_result(rows_in, weight_gate, weight_up, weight_down):
    expert_hidden = (jax.nn.silu(matmul(rows_in, weight_gate)) * matmul(rows_in, weight_up)).astype(
        jnp.bfloat16
    )
    return matmul(expert_hidden, weight_down).astype(jnp.bfloat16)


def exchange_kernel(n, spread, source, landed, send_sem, recv_sem, own_sem):
    me = lax.axis_index("ep")
    barrier = pltpu.get_barrier_semaphore()
    for step in range(1, n):
        pl.semaphore_signal(
            barrier, inc=1, device_id={"ep": lax.rem(me + step, n)}, device_id_type=pl.DeviceIdType.MESH
        )
    own = pltpu.make_async_copy(source if spread else source.at[me], landed.at[me], own_sem)
    own.start()
    pl.semaphore_wait(barrier, n - 1)
    copies = []
    for step in range(1, n):
        target = lax.rem(me + step, n)
        copy = pltpu.make_async_remote_copy(
            src_ref=source if spread else source.at[target],
            dst_ref=landed.at[me],
            send_sem=send_sem.at[step],
            recv_sem=recv_sem.at[step],
            device_id={"ep": target},
            device_id_type=pl.DeviceIdType.MESH,
        )
        copy.start()
        copies.append(copy)
    own.wait()
    for copy in copies:
        copy.wait()


def send(source, shape, spread, ident):
    n = shape[0]
    return pl.pallas_call(
        functools.partial(exchange_kernel, n, spread),
        out_shape=jax.ShapeDtypeStruct(shape, source.dtype),
        in_specs=[pl.BlockSpec(memory_space=pltpu.VMEM)],
        out_specs=pl.BlockSpec(memory_space=pltpu.VMEM),
        scratch_shapes=[
            pltpu.SemaphoreType.DMA((n,)),
            pltpu.SemaphoreType.DMA((n,)),
            pltpu.SemaphoreType.DMA,
        ],
        compiler_params=pltpu.CompilerParams(collective_id=ident, has_side_effects=True),
    )(source)


def exchange(blocks, ident):
    return send(blocks, blocks.shape, False, ident)


def gather(block, ident):
    return send(block, (lax.axis_size("ep"),) + block.shape, True, ident)


def transposed(left, right):
    return lax.dot_general(left, right, (((1,), (1,)), ((), ())), preferred_element_type=jnp.float32)


def state_kernel(per_group, decay, inputs, write, read, carried, updated, mixed):
    row, part = pl.program_id(0), pl.program_id(1)
    heads = carried.shape[1]
    scaled = inputs[0, 0]
    lane = lax.broadcasted_iota(jnp.int32, scaled.shape, 1)
    total = jnp.zeros(scaled.shape, jnp.float32)
    entries = carried.shape[3]
    head_dim = carried.shape[2]
    for group in range(heads // per_group):
        write_row = write[0, 0, group : group + 1]
        spread = jnp.broadcast_to(read[0, 0, group : group + 1], (entries, entries))
        spread_high = spread.astype(jnp.bfloat16)
        spread_low = (spread - spread_high.astype(jnp.float32)).astype(jnp.bfloat16)
        pieces = []
        for head in range(group * per_group, (group + 1) * per_group):
            fresh = (
                carried[0, head] * decay[row, part * heads + head]
                + scaled[:, head : head + 1] * write_row
            )
            updated[0, head] = fresh
            pieces.append(fresh)
        stacked = jnp.concatenate(pieces, axis=0)
        high = stacked.astype(jnp.bfloat16)
        low = (stacked - high.astype(jnp.float32)).astype(jnp.bfloat16)
        columns = transposed(high, spread_high) + transposed(low, spread_high) + transposed(high, spread_low)
        for place in range(per_group):
            head = group * per_group + place
            column = columns[place * head_dim : (place + 1) * head_dim, :heads]
            total = jnp.where(lane == head, column, total)
    mixed[0, 0] = total


def state_step(state, decay_rate, scaled, write_vec, read_vec):
    rows, head_count, head_dim, entries = state.shape
    groups = write_vec.shape[1]
    parts = 2
    heads = head_count // parts
    inputs = scaled.reshape(rows, parts, heads, head_dim).transpose(0, 1, 3, 2)
    vec_shape = (rows, parts, groups // parts, entries)
    part_spec = lambda *dims: pl.BlockSpec((1, 1) + dims, lambda row, part: (row, part, 0, 0))
    state_spec = pl.BlockSpec((1, heads, head_dim, entries), lambda row, part: (row, part, 0, 0))
    next_state, mixed = pl.pallas_call(
        functools.partial(state_kernel, head_count // groups),
        grid=(rows, parts),
        out_shape=(
            jax.ShapeDtypeStruct(state.shape, jnp.float32),
            jax.ShapeDtypeStruct(inputs.shape, jnp.float32),
        ),
        in_specs=[
            pl.BlockSpec(memory_space=pltpu.SMEM),
            part_spec(head_dim, heads),
            part_spec(groups // parts, entries),
            part_spec(groups // parts, entries),
            state_spec,
        ],
        out_specs=(state_spec, part_spec(head_dim, heads)),
    )(decay_rate, inputs, write_vec.reshape(vec_shape), read_vec.reshape(vec_shape), state)
    return next_state, mixed.transpose(0, 1, 3, 2).reshape(rows, head_count, head_dim)


def shards(
    hidden,
    conv_window,
    ssm_state,
    gate_proj,
    input_proj,
    write_proj,
    read_proj,
    step_proj,
    step_bias,
    decay_log,
    decay_shift,
    skip_scale,
    conv_taps,
    conv_bias,
    mix_gain,
    group_gain,
    out_proj,
    ffn_gain,
    router,
    expert_ids,
    expert_gate,
    expert_up,
    expert_down,
    shared_gate,
    shared_up,
    shared_down,
):
    local_rows = hidden.shape[0]
    device_index = lax.axis_index("ep")
    width = hidden.shape[1]
    first_row = device_index * local_rows
    gathered = gather(hidden, 0).reshape(-1, width)
    gathered_wide = gathered.astype(jnp.float32)
    normed = (gathered_wide * row_scale(gathered_wide) * mix_gain).astype(jnp.bfloat16)
    parts = [matmul(normed, proj).astype(jnp.bfloat16) for proj in (gate_proj, input_proj, write_proj, read_proj)]
    outbound = jnp.concatenate(parts, axis=1)
    arrived = exchange(outbound.reshape(-1, local_rows, outbound.shape[1]), 1)
    rows, offset = [], 0
    for part in parts:
        piece = arrived[:, :, offset : offset + part.shape[1]]
        rows.append(piece.transpose(1, 0, 2).reshape(local_rows, -1))
        offset += part.shape[1]
    gate_rows, input_rows, write_rows, read_rows = rows
    hidden_wide = hidden.astype(jnp.float32)
    normed_local = (hidden_wide * row_scale(hidden_wide) * mix_gain).astype(jnp.bfloat16)
    step_raw = matmul(normed_local, step_proj)
    inner_width = gate_rows.shape[1]
    state_span = GROUPS * STATE
    head_count = step_bias.shape[0]
    fresh_row = jnp.concatenate([input_rows, write_rows, read_rows], axis=1)
    window = jnp.concatenate([conv_window, fresh_row[:, None, :]], axis=1)
    convolved = jax.nn.silu(
        jnp.sum(window.astype(jnp.float32) * conv_taps.astype(jnp.float32)[None], axis=1)
        + conv_bias
    )
    head_input = convolved[:, :inner_width].reshape(local_rows, head_count, HEAD_DIM)
    write_vec = convolved[:, inner_width : inner_width + state_span].reshape(
        local_rows, GROUPS, STATE
    )
    read_vec = convolved[:, inner_width + state_span :].reshape(local_rows, GROUPS, STATE)
    step_size = jax.nn.softplus(step_raw + step_bias)
    decay_rate = jnp.exp(decay_shift - step_size * jnp.exp(decay_log))
    next_state, mixed_out = state_step(
        ssm_state, decay_rate, step_size[:, :, None] * head_input, write_vec, read_vec
    )
    mixed_out = mixed_out + skip_scale[None, :, None] * head_input
    mixed_out = mixed_out.reshape(local_rows, inner_width).astype(jnp.bfloat16)
    gated_out = mixed_out.astype(jnp.float32) * jax.nn.silu(gate_rows.astype(jnp.float32))
    blocks = gated_out.reshape(local_rows, GROUPS, -1)
    gated_out = ((blocks * row_scale(blocks)).reshape(local_rows, inner_width) * group_gain).astype(
        jnp.bfloat16
    )
    col_width = out_proj.shape[1]
    resid_cols = lax.dynamic_slice_in_dim(gathered_wide, device_index * col_width, col_width, 1)
    resid_part = (
        resid_cols + matmul(gather(gated_out, 2).reshape(-1, inner_width), out_proj)
    ).astype(jnp.bfloat16)
    resid_all = gather(resid_part, 3).transpose(1, 0, 2).reshape(-1, width)
    gain_part = lax.dynamic_slice_in_dim(ffn_gain, device_index * col_width, col_width, 0)
    shared_part = (resid_part.astype(jnp.float32) * gain_part).astype(jnp.bfloat16)
    shared_pre = jnp.concatenate(
        [matmul(shared_part, shared_gate), matmul(shared_part, shared_up)], axis=1
    ).astype(jnp.bfloat16)
    resid_all_wide = resid_all.astype(jnp.float32)
    scale_all = row_scale(resid_all_wide)
    routed_all = (resid_all_wide * scale_all * ffn_gain).astype(jnp.bfloat16)
    result = expert_result(routed_all, expert_gate[0], expert_up[0], expert_down[0])
    back = exchange(
        jnp.concatenate([result, shared_pre], axis=1).reshape(
            -1, local_rows, width + shared_pre.shape[1]
        ),
        4,
    ).astype(jnp.float32)
    resid_wide = lax.dynamic_slice_in_dim(resid_all_wide, first_row, local_rows, 0)
    norm_scale = lax.dynamic_slice_in_dim(scale_all, first_row, local_rows, 0)
    routed_in = lax.dynamic_slice_in_dim(routed_all, first_row, local_rows, 0)
    scores = jax.nn.sigmoid(matmul(routed_in, router))
    chosen = jnp.any(
        expert_ids[:, :, None] == jnp.arange(router.shape[1], dtype=jnp.int32)[None, None, :], axis=1
    )
    scores = jnp.where(chosen, scores, 0.0)
    weights = routed_scale * scores / jnp.sum(scores, axis=1, keepdims=True)
    routed = jnp.sum(back[:, :, :width] * weights.T[:, :, None], axis=0)
    shared_sum = jnp.sum(back[:, :, width:], axis=0)
    hidden_units = shared_down.shape[0]
    shared_hidden = (
        jax.nn.silu(norm_scale * shared_sum[:, :hidden_units])
        * (norm_scale * shared_sum[:, hidden_units:])
    ).astype(jnp.bfloat16)
    layer_out = (resid_wide + routed + matmul(shared_hidden, shared_down)).astype(jnp.bfloat16)
    return (layer_out, next_state, window[:, 1:])


def solution(mesh):
    placed = (
        P(("grp", "ep"), None),
        P(("grp", "ep"), None, None),
        P(("grp", "ep"), None, None, None),
        P(None, "ep"),
        P(None, "ep"),
        P(None, "ep"),
        P(None, "ep"),
        P(),
        P(),
        P(),
        P(("grp", "ep"), None),
        P(),
        P(),
        P(),
        P(),
        P(),
        P(None, "ep"),
        P(),
        P(),
        P(("grp", "ep"), None),
        P("ep", None, None),
        P("ep", None, None),
        P("ep", None, None),
        P("ep", None),
        P("ep", None),
        P(),
    )
    return jax.shard_map(
        shards,
        mesh=mesh,
        in_specs=placed,
        out_specs=(
            P(("grp", "ep"), None),
            P(("grp", "ep"), None, None, None),
            P(("grp", "ep"), None, None),
        ),
        check_vma=False,
    )
```
